32 devices in a mesh: sp: 4 (over z), fs: 4 (over y, x), tp: 2 (over core).
Axes of the slice: x: 2, y: 2, z: 4, core: 2. Of those that a mesh axis runs over, the one named last changes fastest.
Arguments:
- inputs: bfloat16 [2048, 2048], P(('fs', 'sp'), 'tp'), parts along dimension 0, may hold values from -6 to 6
- norm_gain: float32 [2048], replicated, may hold values from 0.1 to 1.9
- in_ssm: bfloat16 [2048, 1024], P('sp', 'tp'), may hold values from -0.125 to 0.125
- in_query: bfloat16 [2048, 1024], P('sp', 'tp')
- in_key: bfloat16 [2048, 256], P('sp', 'tp')
- in_value: bfloat16 [2048, 256], P('sp', 'tp'), may hold values from -0.125 to 0.125
- decay_rate: float32 [64, 64], P('tp'), as said below
- rotation: float32 [64, 64], P('tp'), may hold values from 0.05 to 3
- input_parts: bfloat16 [2, 64, 64, 16], P(None, 'tp')
- output_parts: bfloat16 [2, 64, 16, 64], P(None, 'tp'), may hold values from -0.5 to 0.5
- skip_scale: float32 [64, 16], P('tp'), may hold values from -4 to 4
- decay_shift: float32 [2048, 64], P(('fs', 'sp'), 'tp'), parts along dimension 0, may hold values from -1 to 0
- sink_logit: float32 [16], P('tp'), may hold values from 2 to 6
- out_state: bfloat16 [1024, 2048], P('tp', 'sp'), may hold values from -0.125 to 0.125
- out_attend: bfloat16 [1024, 2048], P('tp', 'sp'), may hold values from -0.125 to 0.125
Outputs:
- mixed: bfloat16 [2048, 2048], P(('fs', 'sp', 'tp')), parts along dimension 0
The draws below stay inside these ranges and needn't reach their ends.
There are 4 independent parts, one for each index of `fs`. The reference program is written for one: setup_inputs(seed, part) draws one part's arguments, and reference() takes and returns one part's arrays. A program takes and returns all parts, laid end to end along the dimension named above; an argument that names none is the same for every part. Nothing has to cross between parts.
Inputs may be any that keep to these rules, and one draw needn't show every extreme that they name: `decay_rate`: between 1e-5 and 0.1.
All inputs are finite; a program needn't handle non-finite values.
Results may differ from the reference program's by a relative error of at most 0.012.
Values may be sent and summed in bfloat16 or wider, within the bound.
No kernel may reach another device: no remote copies, remote signals or barrier semaphores. Data moves between devices by JAX's collectives and lax.ppermute only.
A program may use at most 64 MiB of HBM per device.

```python
import math
import jax
import jax.numpy as jnp
from jax import lax

D = 2048
GROUPS = 64
GROUP_CH = 16
STATE = 64
Q_HEADS = 16
KV_HEADS = 4
HEAD_DIM = 64
WINDOW = 128
BLOCK = 128
TOK_DEV = 128
LEN = 512
N_SP = 4


def recurrence_law(key):
    mask_key = jax.random.fold_in(key, 11)
    slow_key = jax.random.fold_in(key, 12)
    fast_key = jax.random.fold_in(key, 13)
    part_key = jax.random.fold_in(key, 14)
    portion = 0.5
    slow = jax.random.uniform(mask_key, (GROUPS, STATE), jnp.float32) < portion
    slow_rate = jnp.exp(jax.random.uniform(slow_key, (GROUPS, STATE), jnp.float32, math.log(0.1), math.log(0.4))) / LEN
    fast_rate = jnp.exp(jax.random.uniform(fast_key, (GROUPS, STATE), jnp.float32, math.log(0.02), math.log(0.1)))
    rates = jnp.where(slow, slow_rate, fast_rate)
    spread = jnp.sqrt(1.0 - jnp.exp(-2.0 * rates)) / math.sqrt(GROUP_CH)
    parts = jax.random.normal(part_key, (2, GROUPS, STATE, GROUP_CH), jnp.float32) * spread[None, :, :, None]
    return (rates, parts)


def draw_decay_rate(key, part):
    return recurrence_law(key)[0].astype(jnp.float32)


def draw_input_parts(key, part):
    return recurrence_law(key)[1].astype(jnp.bfloat16)


def attention_law(key):
    noise_key = jax.random.fold_in(key, 22)
    other_key = jax.random.fold_in(key, 23)
    repeat = Q_HEADS // KV_HEADS
    noise = jax.random.normal(noise_key, (D, KV_HEADS, repeat, HEAD_DIM), jnp.float32) / math.sqrt(D)
    keys_part = jax.random.normal(other_key, (D, KV_HEADS, HEAD_DIM), jnp.float32) / math.sqrt(D)
    queries_part = noise
    return (queries_part.reshape(D, Q_HEADS * HEAD_DIM), keys_part.reshape(D, KV_HEADS * HEAD_DIM))


def draw_in_query(key, part):
    return attention_law(key)[0].astype(jnp.bfloat16)


def draw_in_key(key, part):
    return attention_law(key)[1].astype(jnp.bfloat16)


def draw_decay_shift(key, part):
    factor_key = jax.random.fold_in(key, 31)
    noise_key = jax.random.fold_in(key, 32)
    place_key = jax.random.fold_in(key, 33)
    depth_key = jax.random.fold_in(key, 34)
    factor = jnp.exp(jax.random.uniform(factor_key, (LEN // TOK_DEV,), jnp.float32, math.log(0.5), math.log(2.0)))
    per_position = jnp.repeat(factor, TOK_DEV)
    rough = jax.random.uniform(noise_key, (LEN, GROUPS), jnp.float32, 0.25, 1.75)
    background = -(0.3 / LEN) * per_position[:, None] * rough
    places = jax.random.randint(place_key, (2,), 0, LEN)
    struck = jnp.any(jnp.arange(LEN, dtype=jnp.int32)[:, None] == places[None, :], axis=1)
    kept = jax.random.uniform(depth_key, (GROUPS,), jnp.float32, 0.6, 0.8)
    return (background + jnp.where(struck[:, None], jnp.log(kept)[None, :], 0.0)).astype(jnp.float32)


def level_of(rng, shape, cuts, smallest, largest):
    factor_of, own = 1.0, jax.random.fold_in(rng, 6)
    for axis_at, shards_of in cuts:
        heights = jnp.exp(jax.random.uniform(jax.random.fold_in(own, axis_at), (shards_of,), jnp.float32, smallest / len(cuts), largest / len(cuts)))
        factor_of = factor_of * jnp.repeat(heights, shape[axis_at] // shards_of).reshape([-1 if axis == axis_at else 1 for axis in range(len(shape))])
    return factor_of


def normal_values(stream_key, extent, scale, most, cuts=(), held_as=jnp.bfloat16):
    loudness = level_of(stream_key, extent, cuts, -0.22, 0.18) if cuts else 1.0
    entries = jax.random.normal(stream_key, extent, jnp.float32) * scale * loudness
    return jnp.minimum(jnp.maximum(entries, -most), most).astype(held_as)


def setup_inputs(seed: int = 0, part: int = 0) -> dict:
    key_list = jax.random.split(jax.random.key(seed), 16)
    part_keys = jax.random.split(jax.random.fold_in(key_list[15], part), 16)
    return {
        "inputs": normal_values(part_keys[0], (LEN, D), 1.0, 6.0, ((0, 4), (1, 2))),
        "norm_gain": jnp.clip(1.0 + 0.18 * jax.random.normal(key_list[1], (D,), jnp.float32), 0.1, 1.9),
        "in_ssm": normal_values(key_list[2], (D, GROUPS * GROUP_CH), D ** -0.5, 0.125, ((0, 4), (1, 2))),
        "in_query": draw_in_query(jax.random.fold_in(key_list[15], 71), part),
        "in_key": draw_in_key(jax.random.fold_in(key_list[15], 71), part),
        "in_value": normal_values(key_list[5], (D, KV_HEADS * HEAD_DIM), D ** -0.5, 0.125, ((0, 4), (1, 2))),
        "decay_rate": draw_decay_rate(jax.random.fold_in(key_list[15], 71), part),
        "rotation": jnp.clip(0.05 + 2.95 * jax.random.uniform(key_list[7], (GROUPS, STATE), jnp.float32) ** level_of(key_list[7], (GROUPS, STATE), ((0, 2),), -0.2, 0.2), 0.05, 3.0),
        "input_parts": draw_input_parts(jax.random.fold_in(key_list[15], 71), part),
        "output_parts": normal_values(key_list[9], (2, GROUPS, GROUP_CH, STATE), (2 * STATE) ** -0.5, 0.5, ((1, 2),)),
        "skip_scale": normal_values(key_list[10], (GROUPS, GROUP_CH), 1.0, 4.0, ((0, 2),), jnp.float32),
        "decay_shift": draw_decay_shift(jax.random.fold_in(jax.random.fold_in(key_list[15], part), 71), part),
        "sink_logit": jnp.clip(2.0 + 4.0 * jax.random.uniform(key_list[12], (Q_HEADS,), jnp.float32) ** level_of(key_list[12], (Q_HEADS,), ((0, 2),), -0.2, 0.2), 2.0, 6.0),
        "out_state": normal_values(key_list[13], (GROUPS * GROUP_CH, D), (GROUPS * GROUP_CH + Q_HEADS * HEAD_DIM) ** -0.5, 0.125, ((0, 2), (1, 4))),
        "out_attend": normal_values(key_list[14], (Q_HEADS * HEAD_DIM, D), (GROUPS * GROUP_CH + Q_HEADS * HEAD_DIM) ** -0.5, 0.125, ((0, 2), (1, 4))),
    }


epsilon = 1e-06
floor_score = -1e+30

def combine(earlier, later):
    first_re, first_im, state_re, state_im = earlier
    second_re, second_im, input_re, input_im = later
    return (second_re * first_re - second_im * first_im, second_re * first_im + second_im * first_re, second_re * state_re - second_im * state_im + input_re, second_re * state_im + second_im * state_re + input_im)

def input_matrix(decay_rate, rotation, input_parts):
    damped = jnp.exp(-decay_rate)
    lift_re = damped * jnp.cos(rotation) - 1.0
    lift_im = damped * jnp.sin(rotation)
    modulus = decay_rate * decay_rate + rotation * rotation
    factor_re = (rotation * lift_im - decay_rate * lift_re) / modulus
    factor_im = -(rotation * lift_re + decay_rate * lift_im) / modulus
    part_re = input_parts[0].astype(jnp.float32)
    part_im = input_parts[1].astype(jnp.float32)
    joined_re = factor_re[:, :, None] * part_re - factor_im[:, :, None] * part_im
    joined_im = factor_re[:, :, None] * part_im + factor_im[:, :, None] * part_re
    return jnp.concatenate([joined_re, joined_im], axis=1).astype(jnp.bfloat16)

def advance_block(carry, drive, shift, grouped, decay_rate, rotation, output_parts, skip_scale):
    carry_re, carry_im = carry
    width = drive.shape[2] // 2
    magnitude = jnp.exp(shift[:, :, None] - decay_rate[None])
    elements = (magnitude * jnp.cos(rotation)[None], magnitude * jnp.sin(rotation)[None], drive[:, :, :width], drive[:, :, width:])
    decay_re, decay_im, state_re, state_im = lax.associative_scan(combine, elements, axis=0)
    state_re = state_re + decay_re * carry_re[None] - decay_im * carry_im[None]
    state_im = state_im + decay_re * carry_im[None] + decay_im * carry_re[None]
    read_re = output_parts[0].astype(jnp.float32)
    read_im = output_parts[1].astype(jnp.float32)
    result = jnp.einsum('tgp,ghp->tgh', state_re, read_re, precision=lax.Precision.HIGHEST)
    result = result - jnp.einsum('tgp,ghp->tgh', state_im, read_im, precision=lax.Precision.HIGHEST)
    result = result + skip_scale.astype(jnp.float32)[None] * grouped.astype(jnp.float32)
    return ((state_re[-1], state_im[-1]), jax.nn.gelu(result).astype(jnp.bfloat16))

def window_attention(queries, keys_win, values_win, starts, sink_logit):
    window = queries.shape[1]
    scores = jnp.einsum('nqgrd,nkgd->ngrqk', queries.astype(jnp.float32), keys_win.astype(jnp.float32))
    scores = scores * queries.shape[-1] ** (-0.5)
    places = jnp.arange(window, dtype=jnp.int32)[:, None] + window - jnp.arange(2 * window, dtype=jnp.int32)[None, :]
    inside = (places >= 0) & (places < window)
    reach = starts[:, None] - window + jnp.arange(2 * window, dtype=jnp.int32)[None, :] >= 0
    valid = (inside[None] & reach[:, None, :])[:, None, None]
    sinks = sink_logit.astype(jnp.float32).reshape(scores.shape[1], scores.shape[2])[None, :, :, None, None]
    scores = jnp.where(valid, scores, floor_score)
    row_peak = jnp.maximum(lax.optimization_barrier(jnp.max(scores, axis=-1, keepdims=True)), sinks)
    raised = jnp.where(valid, jnp.exp(scores - row_peak), 0.0)
    denominator = lax.optimization_barrier(jnp.sum(raised, axis=-1, keepdims=True)) + jnp.exp(sinks - row_peak)
    weights = (raised / denominator).astype(jnp.bfloat16)
    result = jnp.einsum('ngrqk,nkgd->nqgrd', weights.astype(jnp.float32), values_win.astype(jnp.float32))
    return result.astype(jnp.bfloat16)

def reference(inputs, norm_gain, in_ssm, in_query, in_key, in_value, decay_rate, rotation, input_parts, output_parts, skip_scale, decay_shift, sink_logit, out_state, out_attend):
    length = inputs.shape[0]
    widened = inputs.astype(jnp.float32)
    scale = lax.rsqrt(lax.optimization_barrier(jnp.mean(widened * widened, axis=1, keepdims=True)) + epsilon)
    normed = (widened * scale * norm_gain.astype(jnp.float32)).astype(jnp.bfloat16)
    drive_in = jnp.dot(normed, in_ssm, preferred_element_type=jnp.float32).astype(jnp.bfloat16)
    queries = jnp.dot(normed, in_query, preferred_element_type=jnp.float32).astype(jnp.bfloat16)
    keys_local = jnp.dot(normed, in_key, preferred_element_type=jnp.float32).astype(jnp.bfloat16)
    values = jnp.dot(normed, in_value, preferred_element_type=jnp.float32).astype(jnp.bfloat16)
    in_matrix = input_matrix(decay_rate, rotation, input_parts)
    blocks = length // BLOCK
    grouped = drive_in.reshape(blocks, BLOCK, GROUPS, GROUP_CH)
    shifted = decay_shift.reshape(blocks, BLOCK, GROUPS)

    def advance(carry, pieces):
        grouped_part, shift_part = pieces
        drive = jnp.einsum('tgh,gqh->tgq', grouped_part.astype(jnp.float32), in_matrix.astype(jnp.float32))
        return advance_block(carry, drive, shift_part, grouped_part, decay_rate, rotation, output_parts, skip_scale)
    zero_state = jnp.zeros((GROUPS, STATE), jnp.float32)
    _, state_out = lax.scan(advance, (zero_state, zero_state), (grouped, shifted))
    state_out = state_out.reshape(length, GROUPS * GROUP_CH)
    windows_all = length // WINDOW
    per_device = TOK_DEV // WINDOW
    filler = jnp.zeros((WINDOW, KV_HEADS * HEAD_DIM), jnp.bfloat16)

    def windows(flat):
        split = jnp.concatenate([filler, flat], axis=0).reshape(windows_all + 1, WINDOW, KV_HEADS, HEAD_DIM)
        joined = jnp.concatenate([split[:-1], split[1:]], axis=1)
        return joined.reshape(N_SP, per_device, 2 * WINDOW, KV_HEADS, HEAD_DIM)
    queries_blk = queries.reshape(N_SP, per_device, WINDOW, KV_HEADS, Q_HEADS // KV_HEADS, HEAD_DIM)
    starts = (jnp.arange(windows_all, dtype=jnp.int32) * WINDOW).reshape(N_SP, per_device)
    attended = lax.map(lambda pieces: window_attention(pieces[0], pieces[1], pieces[2], pieces[3], sink_logit), (queries_blk, windows(keys_local), windows(values), starts))
    attend_out = attended.reshape(length, Q_HEADS * HEAD_DIM)
    summed = jnp.dot(state_out, out_state, preferred_element_type=jnp.float32)
    summed = summed + jnp.dot(attend_out, out_attend, preferred_element_type=jnp.float32)
    return summed.astype(jnp.bfloat16)
```

```python
import jax
import jax.numpy as jnp
from jax import lax
from jax.experimental import pallas as pl
from jax.experimental.pallas import tpu as pltpu
from jax.sharding import PartitionSpec as P


GROUP_CH = 16
HEAD_DIM = 64
WINDOW = 128
BLOCK = 128


epsilon = 1e-06
floor_score = -1e30


def prefix(x, axis, join, neutral):
    place = lax.axis_index(axis)
    gathered = jax.tree.map(
        lambda a, kind: lax.all_gather(a.astype(kind), axis),
        x,
        (jnp.bfloat16, jnp.bfloat16, jnp.bfloat16, jnp.bfloat16),
    )
    state = jax.tree.map(lambda a, e: jnp.zeros_like(a) + jnp.asarray(e, a.dtype), x, neutral)

    def one(hop, state):
        return join(
            state,
            jax.tree.map(
                lambda a, own: lax.dynamic_index_in_dim(a, hop, 0, False).astype(own.dtype),
                gathered,
                x,
            ),
        )

    return lax.fori_loop(0, place, one, state)


def from_behind(value, axis, steps):
    count = lax.axis_size(axis)
    initial, last = (max(0, -steps), min(count, count - steps))
    return lax.ppermute(value, axis, [(source, source + steps) for source in range(initial, last)])


def combine(earlier, later):
    first_re, first_im, state_re, state_im = earlier
    second_re, second_im, input_re, input_im = later
    return (
        second_re * first_re - second_im * first_im,
        second_re * first_im + second_im * first_re,
        second_re * state_re - second_im * state_im + input_re,
        second_re * state_im + second_im * state_re + input_im,
    )


def input_matrix(decay_rate, rotation, input_parts):
    damped = jnp.exp(-decay_rate)
    lift_re = damped * jnp.cos(rotation) - 1.0
    lift_im = damped * jnp.sin(rotation)
    modulus = decay_rate * decay_rate + rotation * rotation
    factor_re = (rotation * lift_im - decay_rate * lift_re) / modulus
    factor_im = -(rotation * lift_re + decay_rate * lift_im) / modulus
    part_re = input_parts[0].astype(jnp.float32)
    part_im = input_parts[1].astype(jnp.float32)
    joined_re = factor_re[:, :, None] * part_re - factor_im[:, :, None] * part_im
    joined_im = factor_re[:, :, None] * part_im + factor_im[:, :, None] * part_re
    return jnp.concatenate([joined_re, joined_im], axis=1).astype(jnp.bfloat16)


def window_attention(queries, keys_win, values_win, starts, sink_logit):
    window = queries.shape[1]
    scores = jnp.einsum("nqgrd,nkgd->ngrqk", queries, keys_win, preferred_element_type=jnp.float32)
    scores = scores * queries.shape[-1] ** (-0.5)
    places = (
        jnp.arange(window, dtype=jnp.int32)[:, None]
        + window
        - jnp.arange(2 * window, dtype=jnp.int32)[None, :]
    )
    inside = (places >= 0) & (places < window)
    reach = starts[:, None] - window + jnp.arange(2 * window, dtype=jnp.int32)[None, :] >= 0
    valid = (inside[None] & reach[:, None, :])[:, None, None]
    sinks = sink_logit.reshape(scores.shape[1], scores.shape[2])[None, :, :, None, None]
    scores = jnp.where(valid, scores, floor_score)
    row_peak = jnp.maximum(jnp.max(scores, axis=-1, keepdims=True), sinks)
    raised = jnp.where(valid, jnp.exp(scores - row_peak), 0.0)
    denominator = jnp.sum(raised, axis=-1, keepdims=True) + jnp.exp(sinks - row_peak)
    weights = (raised / denominator).astype(jnp.bfloat16)
    result = jnp.einsum(
        "ngrqk,nkgd->nqgrd", weights, values_win, preferred_element_type=jnp.float32
    )
    return result.astype(jnp.bfloat16)


def body(
    inputs,
    norm_gain,
    in_ssm,
    in_query,
    in_key,
    in_value,
    decay_rate,
    rotation,
    input_parts,
    output_parts,
    skip_scale,
    decay_shift,
    sink_logit,
    out_state,
    out_attend,
):
    gathered = lax.all_gather(inputs, "tp", axis=1, tiled=True)
    length = gathered.shape[0]
    widened = gathered.astype(jnp.float32)
    scale = lax.rsqrt(jnp.mean(widened * widened, axis=1, keepdims=True) + epsilon)
    normed = (widened * scale * norm_gain).astype(jnp.bfloat16)

    def add_rows(pieces):
        return tuple(
            (jnp.dot(normed, piece, preferred_element_type=jnp.float32) for piece in pieces)
        )

    projected = add_rows(
        (
            lax.all_gather(in_ssm, "sp", axis=0, tiled=True),
            lax.all_gather(in_query, "sp", axis=0, tiled=True),
            lax.all_gather(in_key, "sp", axis=0, tiled=True),
            lax.all_gather(in_value, "sp", axis=0, tiled=True),
        )
    )
    drive_in, queries, keys_local, values = [piece.astype(jnp.bfloat16) for piece in projected]
    groups = decay_rate.shape[0]
    state_dim = decay_rate.shape[1]
    channels = groups * GROUP_CH
    highest = lax.Precision.HIGHEST
    drive_cols = jnp.transpose(drive_in).reshape(groups, GROUP_CH, length)
    in_matrix = input_matrix(decay_rate, rotation, input_parts)
    drive = jnp.einsum("gqh,ght->gqt", in_matrix, drive_cols, preferred_element_type=jnp.float32)
    shift_cols = jnp.transpose(decay_shift)
    running = jnp.cumsum(shift_cols, axis=1)
    total_shift = running[:, -1]
    remain = length - 1.0 - jnp.arange(length, dtype=jnp.float32)
    to_end = (total_shift[:, None] - running)[:, None, :] - decay_rate[:, :, None] * remain[
        None, None, :
    ]
    fade = jnp.exp(to_end)
    turn = rotation[:, :, None] * remain[None, None, :]
    weight_re = fade * jnp.cos(turn)
    weight_im = fade * jnp.sin(turn)
    drive_re = drive[:, :state_dim]
    drive_im = drive[:, state_dim:]
    final_re = jnp.sum(weight_re * drive_re - weight_im * drive_im, axis=2)
    final_im = jnp.sum(weight_re * drive_im + weight_im * drive_re, axis=2)
    overall = jnp.exp(total_shift[:, None] - decay_rate * length)
    nothing = jnp.zeros_like(final_re)
    carried = prefix(
        (
            overall * jnp.cos(rotation * length),
            overall * jnp.sin(rotation * length),
            final_re,
            final_im,
        ),
        "sp",
        combine,
        (jnp.ones_like(final_re), nothing, nothing, nothing),
    )
    key_heads = keys_local.shape[1] // HEAD_DIM
    query_heads = queries.shape[1] // HEAD_DIM
    windows_dev = length // WINDOW
    previous = from_behind((keys_local, values), "sp", 1)

    def windows(flat, before):
        split = jnp.concatenate([before, flat], axis=0).reshape(
            windows_dev + 1, WINDOW, key_heads, HEAD_DIM
        )
        return jnp.concatenate([split[:-1], split[1:]], axis=1)

    offset = lax.axis_index("sp") * length
    starts = offset + jnp.arange(windows_dev, dtype=jnp.int32) * WINDOW
    queries_blk = queries.reshape(
        windows_dev, WINDOW, key_heads, query_heads // key_heads, HEAD_DIM
    )
    attended = window_attention(
        queries_blk,
        windows(keys_local, previous[0]),
        windows(values, previous[1]),
        starts,
        sink_logit,
    )
    attend_out = attended.reshape(length, query_heads * HEAD_DIM)
    blocks = length // BLOCK
    triangle = (
        jnp.arange(BLOCK, dtype=jnp.int32)[:, None] <= jnp.arange(BLOCK, dtype=jnp.int32)[None, :]
    ).astype(jnp.float32)
    offsets = jnp.arange(BLOCK, dtype=jnp.float32)
    centre = BLOCK // 2
    read_re = output_parts[0].astype(jnp.float32)
    read_im = output_parts[1].astype(jnp.float32)
    angle = rotation[:, :, None] * (offsets - centre)[None, None, :]
    cos_angle = jnp.cos(angle)
    sin_angle = jnp.sin(angle)
    phase = rotation[:, :, None] * (offsets + 1.0)[None, None, :]
    cos_phase = jnp.cos(phase)
    sin_phase = jnp.sin(phase)

    def advance(carry, pieces):
        carry_re, carry_im = carry
        part_re, part_im, shift_part, grouped_part = pieces
        level = jnp.dot(shift_part, triangle, precision=highest)
        log_from = level[:, None, :] - decay_rate[:, :, None] * (offsets + 1.0)[None, None, :]
        relative = log_from - log_from[:, :, centre : centre + 1]
        shrink = jnp.exp(-relative)
        lift_re = shrink * (part_re * cos_angle + part_im * sin_angle)
        lift_im = shrink * (part_im * cos_angle - part_re * sin_angle)
        prefix_re = jnp.dot(lift_re.reshape(groups * state_dim, BLOCK), triangle, precision=highest)
        prefix_im = jnp.dot(lift_im.reshape(groups * state_dim, BLOCK), triangle, precision=highest)
        prefix_re = prefix_re.reshape(groups, state_dim, BLOCK)
        prefix_im = prefix_im.reshape(groups, state_dim, BLOCK)
        grow = jnp.exp(relative)
        from_start = jnp.exp(log_from)
        keep_re = from_start * cos_phase
        keep_im = from_start * sin_phase
        state_re = grow * (prefix_re * cos_angle - prefix_im * sin_angle)
        state_im = grow * (prefix_im * cos_angle + prefix_re * sin_angle)
        state_re = state_re + keep_re * carry_re[:, :, None] - keep_im * carry_im[:, :, None]
        state_im = state_im + keep_re * carry_im[:, :, None] + keep_im * carry_re[:, :, None]
        result = jnp.einsum("ghp,gpt->ght", read_re, state_re, precision=highest)
        result = result - jnp.einsum("ghp,gpt->ght", read_im, state_im, precision=highest)
        result = result + skip_scale[:, :, None] * grouped_part.astype(jnp.float32)
        return ((state_re[:, :, -1], state_im[:, :, -1]), jax.nn.gelu(result).astype(jnp.bfloat16))

    drive_blocks = jnp.transpose(drive.reshape(groups, 2 * state_dim, blocks, BLOCK), (2, 0, 1, 3))
    shift_blocks = jnp.transpose(shift_cols.reshape(groups, blocks, BLOCK), (1, 0, 2))
    grouped_blocks = jnp.transpose(
        drive_cols.reshape(groups, GROUP_CH, blocks, BLOCK), (2, 0, 1, 3)
    )
    _, state_blocks = lax.scan(
        advance,
        (carried[2], carried[3]),
        (
            drive_blocks[:, :, :state_dim],
            drive_blocks[:, :, state_dim:],
            shift_blocks,
            grouped_blocks,
        ),
    )
    state_out = jnp.transpose(state_blocks, (0, 3, 1, 2)).reshape(length, channels)
    column_state, column_attend = (
        lax.all_gather(out_state, "sp", axis=1, tiled=True),
        lax.all_gather(out_attend, "sp", axis=1, tiled=True),
    )
    result = jnp.dot(state_out, column_state, preferred_element_type=jnp.float32)
    return lax.psum_scatter(
        (result + jnp.dot(attend_out, column_attend, preferred_element_type=jnp.float32)).astype(
            jnp.bfloat16
        ),
        "tp",
        scatter_dimension=0,
        tiled=True,
    )


def across(value, axis, distance):
    count = lax.axis_size(axis)
    return lax.ppermute(value, axis, [(place, place ^ distance) for place in range(count)])


def spread(piece, order):
    count = lax.axis_size("fs")
    if order is None:
        return [piece] + [across(piece, "fs", j) for j in range(1, count)]
    held, names = [piece], [0]
    for bit in order:
        sent = held[0] if len(held) == 1 else jnp.concatenate(held, axis=0)
        came = across(sent, "fs", bit)
        rows = piece.shape[0]
        held = held + [came[i * rows : (i + 1) * rows] for i in range(len(names))]
        names = names + [name ^ bit for name in names]
    return [held[names.index(j)] for j in range(count)]


def half(value, axis, place):
    size = value.shape[axis] // 2
    return lax.dynamic_slice_in_dim(value, place * size, size, axis)


def assemble(weights, ids, pieces, rows, part):
    own, others = pieces[0], pieces[1:]
    here, column = ids[0], ids[1]
    weights[pl.ds(pl.multiple_of(here * rows, 8), rows), :] = own[...]
    count = rows // part
    for at, piece in enumerate(others):
        hop, turn = at // count + 1, at % count
        first = (here ^ hop) * rows + (column ^ turn) * part
        weights[pl.ds(pl.multiple_of(first, 8), part), :] = piece[...]


def project_kernel(ids, normed, *refs):
    pieces, result, weights = refs[:-2], refs[-2], refs[-1]
    assemble(weights, ids, pieces, pieces[0].shape[0], pieces[1].shape[0])
    result[...] = jnp.dot(
        normed[...], weights[...], preferred_element_type=jnp.float32
    ).astype(jnp.bfloat16)


def kernel_call(body, ids, values, shapes, scratch=()):
    return pl.pallas_call(
        body,
        out_shape=shapes,
        in_specs=[pl.BlockSpec(memory_space=pltpu.SMEM)]
        + [pl.BlockSpec(memory_space=pltpu.VMEM)] * len(values),
        out_specs=jax.tree.map(lambda _: pl.BlockSpec(memory_space=pltpu.VMEM), shapes),
        scratch_shapes=list(scratch),
        compiler_params=pltpu.CompilerParams(vmem_limit_bytes=48 * 1024 * 1024),
    )(ids, *values)


def gather_kernel(ids, drive_in, lift_mats, lift_cos, lift_sin, grow_cos, grow_sin, entry, pref, final):
    length = drive_in.shape[0]
    lanes = lift_cos.shape[1]
    unit = 128
    step = jnp.where(
        lax.broadcasted_iota(jnp.int32, (BLOCK, 2 * BLOCK), 0)
        >= lax.broadcasted_iota(jnp.int32, (BLOCK, 2 * BLOCK), 1) % BLOCK,
        1.0,
        0.0,
    ).astype(jnp.bfloat16)
    per = lift_mats.shape[1]
    groups_unit = lanes // unit
    for i in range(groups_unit):
        cols = pl.ds(i * unit, unit)
        chans = pl.ds((i * unit * drive_in.shape[1] // lanes) // per * per, per)
        matrix = jnp.concatenate([lift_mats[0, :, cols], lift_mats[1, :, cols]], axis=1)
        last_re = last_im = None
        for block in range(length // BLOCK):
            rows = pl.ds(block * BLOCK, BLOCK)
            drive = jnp.dot(drive_in[rows, chans], matrix, preferred_element_type=jnp.float32)
            part_re, part_im = drive[:, :unit], drive[:, unit:]
            lc, ls = lift_cos[rows, cols], lift_sin[rows, cols]
            lifted = jnp.concatenate([part_re * lc + part_im * ls, part_im * lc - part_re * ls], axis=1)
            high = lifted.astype(jnp.bfloat16)
            low = (lifted - high.astype(jnp.float32)).astype(jnp.bfloat16)
            sums = jnp.dot(step, jnp.concatenate([high, low], axis=0), preferred_element_type=jnp.float32)
            pref[rows, pl.ds(2 * i * unit, 2 * unit)] = sums
            end = block * BLOCK + BLOCK - 1
            end_re, end_im = sums[BLOCK - 1 :, :unit], sums[BLOCK - 1 :, unit:]
            if last_re is not None:
                e_re, e_im = entry[0, pl.ds(block, 1), cols], entry[1, pl.ds(block, 1), cols]
                end_re, end_im = (
                    end_re + e_re * last_re - e_im * last_im,
                    end_im + e_re * last_im + e_im * last_re,
                )
            g_re, g_im = grow_cos[pl.ds(end, 1), cols], grow_sin[pl.ds(end, 1), cols]
            last_re, last_im = end_re * g_re - end_im * g_im, end_im * g_re + end_re * g_im
        final[pl.ds(0, 1), cols] = last_re
        final[pl.ds(1, 1), cols] = last_im


def read_kernel(ids, drive_in, pref, carried, read_mats, skip, grow_cos, grow_sin, entry, result):
    length, channels = drive_in.shape
    lanes = grow_cos.shape[1]
    unit = 128
    per = read_mats.shape[2]
    inner = lanes * per // channels // unit
    for o in range(channels // per):
        last = [None] * inner
        chans = pl.ds(o * per, per)
        for block in range(length // BLOCK):
            rows = pl.ds(block * BLOCK, BLOCK)
            total = jnp.zeros((BLOCK, per), jnp.float32)
            for k in range(inner):
                i = o * inner + k
                cols = pl.ds(i * unit, unit)
                if block == 0:
                    last_re, last_im = carried[pl.ds(0, 1), cols], carried[pl.ds(1, 1), cols]
                else:
                    last_re, last_im = last[k]
                e_re, e_im = entry[0, pl.ds(block, 1), cols], entry[1, pl.ds(block, 1), cols]
                p_re = pref[rows, pl.ds(2 * i * unit, unit)] + (e_re * last_re - e_im * last_im)
                p_im = pref[rows, pl.ds((2 * i + 1) * unit, unit)] + (e_re * last_im + e_im * last_re)
                gc, gs = grow_cos[rows, cols], grow_sin[rows, cols]
                s_re, s_im = p_re * gc - p_im * gs, p_im * gc + p_re * gs
                last[k] = (s_re[BLOCK - 1 :], s_im[BLOCK - 1 :])
                state = jnp.concatenate([s_re, s_im], axis=1).astype(jnp.bfloat16)
                reads = jnp.concatenate([read_mats[0, cols, :], read_mats[1, cols, :]], axis=0)
                total = total + jnp.dot(state, reads, preferred_element_type=jnp.float32)
            total = total + skip[:, chans] * drive_in[rows, chans].astype(jnp.float32)
            result[rows, chans] = jax.nn.gelu(total).astype(jnp.bfloat16)


def out_kernel(ids, state_out, attend_out, *refs):
    n_pieces = len(refs) - 2
    pieces, result, weights = refs[:n_pieces], refs[n_pieces], refs[n_pieces + 1]
    here, column, core = ids[0], ids[1], ids[2]
    rows, width = pieces[0].shape
    part = pieces[1].shape[0]
    count = rows // part
    cut = state_out.shape[0] // 4
    pick = lambda ref: jnp.concatenate(
        [ref[pl.ds(pl.multiple_of((2 * i + core) * cut, 8), cut), :] for i in range(2)], axis=0
    )
    active = jnp.concatenate([pick(state_out), pick(attend_out)], axis=1)
    others = pieces[1:]
    for hop in range(result.shape[1] // width):
        if hop == 0:
            matrix = pieces[0][...]
        else:
            for turn in range(count):
                piece = others[(hop - 1) * count + turn]
                weights[pl.ds(pl.multiple_of((column ^ turn) * part, 8), part), :] = piece[...]
            matrix = weights[...]
        place = pl.multiple_of((here ^ hop) * width, 128)
        result[:, pl.ds(place, width)] = jnp.dot(
            active, matrix, preferred_element_type=jnp.float32
        ).astype(jnp.bfloat16)


def paired_body(
    inputs,
    norm_gain,
    in_ssm,
    in_query,
    in_key,
    in_value,
    decay_rate,
    rotation,
    input_parts,
    output_parts,
    skip_scale,
    decay_shift,
    sink_logit,
    out_state,
    out_attend,
):
    n_sp, n_fs = lax.axis_size("sp"), lax.axis_size("fs")
    here, column, core = (lax.axis_index(name) for name in ("sp", "fs", "tp"))
    side, pair = here % 2, here // 2
    bf16 = jnp.bfloat16

    met = across(inputs, "sp", 1)
    shift_met = across(decay_shift, "sp", 1)

    def in_order(own, other):
        return jnp.concatenate(
            [jnp.where(side == 0, own, other), jnp.where(side == 0, other, own)], axis=0
        )

    in_halves = jnp.stack(
        [
            jnp.concatenate(
                [
                    w[:, i * w.shape[1] // 2 : (i + 1) * w.shape[1] // 2]
                    for w in (in_ssm, in_query, in_key, in_value)
                ],
                axis=1,
            )
            for i in range(2)
        ]
    )
    out_halves = jnp.stack(
        [
            jnp.concatenate(
                [w[i * w.shape[0] // 2 : (i + 1) * w.shape[0] // 2] for w in (out_state, out_attend)],
                axis=0,
            )
            for i in range(2)
        ]
    )

    def share(halves, hop):
        part = halves.shape[1] // n_fs
        return lax.dynamic_slice(
            halves, (side ^ (hop & 1), column * part, 0), (1, part, halves.shape[2])
        )[0]

    hops = range(1, n_sp)
    in_came = [across(share(in_halves, hop), "sp", hop) for hop in hops]
    out_came = [across(share(out_halves, hop), "sp", hop) for hop in hops]
    orders = [(1, 2), (2, 1), None]
    in_pieces = [lax.dynamic_index_in_dim(in_halves, side, 0, False)]
    for at, piece in enumerate(in_came):
        order = orders[at % 3] if n_fs == 4 else None
        in_pieces = in_pieces + spread(piece, order)
    out_part = out_came[0].shape[0]
    out_spread = spread(jnp.concatenate(out_came, axis=1), None)
    width = out_halves.shape[2]
    out_pieces = [lax.dynamic_index_in_dim(out_halves, side, 0, False)]
    for at in range(n_sp - 1):
        out_pieces = out_pieces + [p[:, at * width : (at + 1) * width] for p in out_spread]

    gathered = lax.all_gather(in_order(inputs, met), "tp", axis=1, tiled=True)
    length = gathered.shape[0]
    widened = gathered.astype(jnp.float32)
    scale = lax.rsqrt(jnp.mean(widened * widened, axis=1, keepdims=True) + epsilon)
    normed = (widened * scale * norm_gain).astype(bf16)

    rate = half(decay_rate, 0, side)
    turn = half(rotation, 0, side)
    groups, state_dim = rate.shape
    lanes = groups * state_dim
    shift = half(in_order(decay_shift, shift_met), 1, side)
    blocks = length // BLOCK
    centre = BLOCK // 2
    level = jnp.cumsum(shift.reshape(blocks, BLOCK, groups), axis=1)
    offsets = jnp.arange(BLOCK, dtype=jnp.float32)[:, None]
    rate_row, turn_row = rate.reshape(1, lanes), turn.reshape(1, lanes)
    relative = jnp.repeat(level - level[:, centre : centre + 1], state_dim, axis=2) - (
        rate_row * (offsets - centre)
    )
    angle = turn_row * (offsets - centre)
    cos_angle, sin_angle = jnp.cos(angle), jnp.sin(angle)
    shrink, grow = jnp.exp(-relative), jnp.exp(relative)
    flat = lambda a: a.reshape(length, lanes)
    lift_cos, lift_sin = flat(shrink * cos_angle), flat(shrink * sin_angle)
    grow_cos, grow_sin = flat(grow * cos_angle), flat(grow * sin_angle)
    from_start = jnp.exp(
        jnp.repeat(level[:, centre], state_dim, axis=1) - rate_row * (centre + 1.0)
    )
    entry = jnp.stack(
        [from_start * jnp.cos(turn_row * (centre + 1.0)), from_start * jnp.sin(turn_row * (centre + 1.0))]
    )
    in_matrix = input_matrix(rate, turn, half(input_parts, 1, side))
    per_unit = 128 // GROUP_CH
    mine = (
        jnp.arange(128, dtype=jnp.int32)[:, None] // GROUP_CH
        == (jnp.arange(lanes, dtype=jnp.int32)[None, :] // state_dim) % per_unit
    )
    lift_rows = jnp.transpose(in_matrix.reshape(groups, 2, state_dim, GROUP_CH), (1, 3, 0, 2))
    lift_mats = jnp.where(mine, jnp.tile(lift_rows.reshape(2, GROUP_CH, lanes), (1, per_unit, 1)), 0)
    read = half(output_parts, 1, side)
    read = jnp.stack([read[0], -read[1]])
    read_rows = jnp.transpose(read, (0, 1, 3, 2)).reshape(2, lanes, GROUP_CH)
    read_mats = jnp.where(jnp.transpose(mine), jnp.tile(read_rows, (1, 1, per_unit)), 0)
    skip = half(skip_scale, 0, side).reshape(1, groups * GROUP_CH)

    ids = jnp.stack([here, column, core]).astype(jnp.int32)
    total = in_pieces[0].shape[1]
    projected = kernel_call(
        project_kernel,
        ids,
        [normed] + in_pieces,
        jax.ShapeDtypeStruct((length, total), bf16),
        [pltpu.VMEM((normed.shape[1], total), bf16)],
    )
    cuts = [w.shape[1] // 2 for w in (in_ssm, in_query, in_key, in_value)]
    ends = [sum(cuts[: i + 1]) for i in range(4)]
    drive_in, queries, keys_local, values = (
        projected[:, end - cut : end] for cut, end in zip(cuts, ends)
    )
    keys_values = projected[length - WINDOW :, ends[1] :]

    onward = [(place, place + 2) for place in range(n_sp - 2)]
    before = lax.ppermute(keys_values, "sp", onward)

    pref, final = kernel_call(
        gather_kernel,
        ids,
        [drive_in, lift_mats, lift_cos, lift_sin, grow_cos, grow_sin, entry],
        (
            jax.ShapeDtypeStruct((length, 2 * lanes), jnp.float32),
            jax.ShapeDtypeStruct((2, lanes), jnp.float32),
        ),
    )
    carried = jnp.zeros_like(final)
    sent = final.astype(bf16)
    span_re = span_im = None
    for far in range(1, n_sp // 2):
        ways = [(place, place + 2 * far) for place in range(n_sp - 2 * far)]
        state = lax.ppermute(sent, "sp", ways).astype(jnp.float32)
        if far == 1:
            carried = carried + state
        else:
            carried = carried + jnp.stack(
                [span_re * state[0] - span_im * state[1], span_re * state[1] + span_im * state[0]]
            )
        if far + 1 < n_sp // 2:
            whole = lax.ppermute(jnp.sum(shift, axis=0), "sp", ways)
            fade = jnp.exp(jnp.repeat(whole, state_dim) - rate_row[0] * length)
            by_re, by_im = fade * jnp.cos(turn_row[0] * length), fade * jnp.sin(turn_row[0] * length)
            if span_re is None:
                span_re, span_im = by_re, by_im
            else:
                span_re, span_im = span_re * by_re - span_im * by_im, span_re * by_im + span_im * by_re

    key_heads = keys_local.shape[1] // HEAD_DIM
    query_heads = queries.shape[1] // HEAD_DIM
    windows_dev = length // WINDOW

    def windows(flat_rows, earlier):
        split = jnp.concatenate([earlier, flat_rows], axis=0).reshape(
            windows_dev + 1, WINDOW, key_heads, HEAD_DIM
        )
        return jnp.concatenate([split[:-1], split[1:]], axis=1)

    starts = pair * length + jnp.arange(windows_dev, dtype=jnp.int32) * WINDOW
    attended = window_attention(
        queries.reshape(windows_dev, WINDOW, key_heads, query_heads // key_heads, HEAD_DIM),
        windows(keys_local, before[:, : cuts[2]]),
        windows(values, before[:, cuts[2] :]),
        starts,
        half(sink_logit, 0, side),
    )
    attend_out = attended.reshape(length, query_heads * HEAD_DIM)
    state_out = kernel_call(
        read_kernel,
        ids,
        [drive_in, pref, carried, read_mats, skip, grow_cos, grow_sin, entry],
        jax.ShapeDtypeStruct((length, groups * GROUP_CH), bf16),
    )

    def sums_for(which):
        return kernel_call(
            out_kernel,
            jnp.stack([here, column, which]).astype(jnp.int32),
            [state_out, attend_out] + out_pieces,
            jax.ShapeDtypeStruct((length // 2, n_sp * width), bf16),
            [pltpu.VMEM((out_pieces[0].shape[0], width), bf16)],
        )

    theirs = across(sums_for(1 - core), "tp", 1)
    ours = sums_for(core).astype(jnp.float32) + theirs.astype(jnp.float32)
    cut = length // 4
    away = lax.dynamic_slice_in_dim(ours, (1 - side) * cut, cut, 0).astype(bf16)
    back = across(away, "sp", 1)
    kept = lax.dynamic_slice_in_dim(ours, side * cut, cut, 0)
    return (kept + back.astype(jnp.float32)).astype(bf16)


def solution(mesh):
    n_sp, n_fs, n_tp = mesh.shape["sp"], mesh.shape["fs"], mesh.shape["tp"]
    paired = n_tp == 2 and n_sp in (2, 4, 8) and n_fs in (1, 2, 4, 8)
    return jax.shard_map(
        paired_body if paired else body,
        mesh=mesh,
        in_specs=(
            P(("fs", "sp"), "tp"),
            P(),
            P("sp", "tp"),
            P("sp", "tp"),
            P("sp", "tp"),
            P("sp", "tp"),
            P("tp", None),
            P("tp", None),
            P(None, "tp", None, None),
            P(None, "tp", None, None),
            P("tp", None),
            P(("fs", "sp"), "tp"),
            P("tp"),
            P("tp", "sp"),
            P("tp", "sp"),
        ),
        out_specs=P(("fs", "sp", "tp"), None),
        check_vma=False,
    )
```
